32 devices in a mesh: sp: 8 (over z, y), tp: 4 (over x, core).
Axes of the slice: x: 2, y: 2, z: 4, core: 2. Of those that a mesh axis runs over, the one named last changes fastest.
Arguments:
- gate_in: bfloat16 [4096, 2048], P('sp', 'tp'), may hold values from -6 to 6
- value_in: bfloat16 [4096, 2048], P('sp', 'tp'), may hold values from -6 to 6
- gate_out: bfloat16 [4096, 2048], P('sp', 'tp'), may hold values from -6 to 6
- conv_taps: float32 [3, 2048], P(None, 'tp'), may hold values from -3.5 to 3.5
- proj_weight: bfloat16 [2048, 2048], P('tp'), may hold values from -0.125 to 0.125
- residual: bfloat16 [4096, 2048], P(('sp', 'tp')), may hold values from -6 to 6
- norm_gain: float32 [2048], replicated, may hold values from 0.1 to 1.9
- routes: int32 [4096, 2], P('sp'), may hold values from 0 to 7, all different within a row; in each aligned block of 128 rows (0 to 127, 128 to 255, ...) at most 64 rows name the same one
- route_weight: float32 [4096, 2], P('sp'), may hold values from 0.1 to 0.9
- expert_gate: bfloat16 [8, 2048, 2048], P('sp', None, 'tp'), may hold values from -0.125 to 0.125
- expert_up: bfloat16 [8, 2048, 2048], P('sp', None, 'tp'), may hold values from -0.125 to 0.125
- expert_down: bfloat16 [8, 2048, 2048], P('sp', 'tp'), may hold values from -0.125 to 0.125
Outputs:
- layer_out: bfloat16 [4096, 2048], P(('sp', 'tp'))
The draws below stay inside these ranges and needn't reach their ends.
Inputs may be any that keep to these rules, and one draw needn't show every extreme that they name: `routes`: A token's 2 experts differ. In each aligned block of 128 tokens no expert is named by more than 64 tokens, a bound that some block reaches.
All inputs are finite; a program needn't handle non-finite values.
Results may differ from the reference program's by a relative error of at most 0.012.
Values may be sent and summed in bfloat16 or wider, within the bound.
No kernel may reach another device: no remote copies, remote signals or barrier semaphores. Data moves between devices by JAX's collectives and lax.ppermute only.
A program may use at most 128 MiB of HBM per device.

```python
import math
import jax
import jax.numpy as jnp
import numpy as np
from jax import lax

D = 2048
FE = 2048
TOP = 2
TAPS = 3
TOK_DEV = 512
TOKQ = 128
EXPERTS = 8
CAPQ = 64
TOKENS = 4096
N_SP = 8
N_TP = 4


def levels(key, shape, shards, least, largest):
    gain, own = 1.0, jax.random.fold_in(key, 6)
    for position, blocks in shards:
        heights = jnp.exp(jax.random.uniform(jax.random.fold_in(own, position), (blocks,), jnp.float32, least / len(shards), largest / len(shards)))
        gain = gain * jnp.repeat(heights, shape[position] // blocks).reshape([-1 if axis == position else 1 for axis in range(len(shape))])
    return gain


def routed_block(key, own, number, rows, count, top, bound, lean):
    sequence = jax.random.permutation(key, count)
    heavy_load, ordinary = shares(count, rows * top, bound, lean, True), shares(count, rows * top, bound, lean, False)
    places = jnp.arange(count)

    def named(lengths, rotation):
        used = int((lengths > 0).sum())
        fixed = max(1, used // 4)
        moved = fixed + (places - fixed + rotation * (used - fixed)) % max(1, count - fixed)
        return jnp.zeros((count,), jnp.int32).at[sequence[jnp.where(places < fixed, places, moved)]].set(jnp.asarray(lengths, jnp.int32))

    lengths = jnp.where(number % 4 == 0, named(heavy_load, number // 4), named(ordinary, number - number // 4 - 1))
    mixed = jax.random.permutation(jax.random.fold_in(own, 3), count)
    giver, sink = mixed[0:count // 2 * 2:2], mixed[1:count // 2 * 2:2]
    slack = jnp.minimum(lengths[giver] - 1, bound - lengths[sink]) // 2
    slack = jnp.where((giver == sequence[0]) | (sink == sequence[0]) | (lengths[sink] == 0), 0, jnp.maximum(slack, 0))
    moved = jax.random.randint(jax.random.fold_in(own, 4), (count // 2,), 0, 1 << 20) % (slack + 1)
    lengths = lengths.at[giver].add(-moved).at[sink].add(moved)
    items = jnp.searchsorted(jnp.cumsum(lengths), jnp.arange(rows * top), side="right").astype(jnp.int32)
    table = items.reshape(top, rows).T
    table = table[jax.random.permutation(jax.random.fold_in(own, 1), rows)]
    rotation = jax.random.randint(jax.random.fold_in(own, 2), (rows, 1), 0, top)
    return jnp.take_along_axis(table, (jnp.arange(top)[None, :] + rotation) % top, axis=1)


def shares(count, total, most, slope, full):
    loads = [(1 << 20) // math.isqrt(rank ** slope) + 1 for rank in range(1, count + 1)]
    largest = most if full else min(most, max(-(-total // count), total * loads[0] // sum(loads)))
    least = 1 if total - largest >= count - 1 else 0
    given, rest = [largest] + [least] * (count - 1), total - largest - least * (count - 1)
    while rest > 0:
        candidates = [i for i in range(1, count) if given[i] < largest] or [i for i in range(1, count) if given[i] < most]
        pool, left = sum([loads[i] for i in candidates]), rest
        for i in candidates:
            extra = min(most - given[i], max(1, left * loads[i] // pool), rest)
            given[i] = given[i] + extra
            rest = rest - extra
    return np.array(given)


def bell_draw(key, extent, spread, reach, cuts=(), kind=jnp.bfloat16):
    array = jax.random.normal(key, extent, jnp.float32) * spread
    if len(cuts) > 0:
        array = levels(key, extent, cuts, -0.22, 0.18) * array
    return jnp.clip(array, min=-reach, max=reach).astype(kind)


def setup_inputs(seed: int = 0) -> dict:
    key_list = jax.random.split(jax.random.key(seed), 13)
    gate_in = bell_draw(key_list[0], (TOKENS, D), 1.0, 6.0, ((0, 8), (1, 4)))
    value_in = bell_draw(key_list[1], (TOKENS, D), 1.0, 6.0, ((0, 8), (1, 4)))
    gate_out = bell_draw(key_list[2], (TOKENS, D), 1.0, 6.0, ((0, 8), (1, 4)))
    conv_taps = bell_draw(key_list[3], (TAPS, D), TAPS ** -0.5, 3.5, ((1, 4),), jnp.float32)
    proj_weight = bell_draw(key_list[4], (D, D), D ** -0.5, 0.125, ((0, 4),))
    residual = bell_draw(key_list[5], (TOKENS, D), 1.0, 6.0, ((0, 32),))
    norm_gain = jnp.clip(1.0 + 0.18 * jax.random.normal(key_list[6], (D,), jnp.float32), 0.1, 1.9)
    routes_keys = jax.random.split(jax.random.fold_in(key_list[7], 1), TOKENS // TOKQ)
    routes_turns = jax.random.permutation(jax.random.fold_in(key_list[7], 3), TOKENS // TOKQ)
    routes = jax.vmap(lambda own, number: routed_block(jax.random.fold_in(key_list[7], 2), own, number, TOKQ, EXPERTS, TOP, CAPQ, 2))(routes_keys, routes_turns).reshape((TOKENS, TOP))
    route_weight = jnp.clip(0.1 + 0.79999997 * jax.random.uniform(key_list[8], (TOKENS, TOP), jnp.float32) ** levels(key_list[8], (TOKENS, TOP), ((0, 8),), -0.2, 0.2), 0.1, 0.9)
    expert_gate = bell_draw(key_list[9], (EXPERTS, D, FE), D ** -0.5, 0.125, ((0, 8), (2, 4)))
    expert_up = bell_draw(key_list[10], (EXPERTS, D, FE), D ** -0.5, 0.125, ((0, 8), (2, 4)))
    expert_down = bell_draw(key_list[11], (EXPERTS, FE, D), FE ** -0.5, 0.125, ((0, 8), (1, 4)))
    return dict(gate_in=gate_in, value_in=value_in, gate_out=gate_out, conv_taps=conv_taps, proj_weight=proj_weight, residual=residual, norm_gain=norm_gain, routes=routes, route_weight=route_weight, expert_gate=expert_gate, expert_up=expert_up, expert_down=expert_down)


def rounded(values):
    return lax.optimization_barrier(values.astype(jnp.bfloat16)).astype(jnp.float32)

def slot_numbers(route_ids, block_rows, expert_count):
    block_count = route_ids.shape[0] // block_rows
    flat_ids = route_ids.reshape(block_count, block_rows * route_ids.shape[1])
    one_hot = (flat_ids[:, :, None] == jnp.arange(expert_count, dtype=jnp.int32)[None, None, :]).astype(jnp.int32)
    before = jnp.cumsum(one_hot, axis=1) - one_hot
    return lax.optimization_barrier(jnp.sum(before * one_hot, axis=2)).reshape(route_ids.shape).astype(jnp.int32)

def normalize(hidden_rows, norm_gain):
    inverse = lax.rsqrt(lax.optimization_barrier(jnp.mean(hidden_rows * hidden_rows, axis=-1, keepdims=True)) + 1e-05)
    return (hidden_rows * inverse * norm_gain.astype(jnp.float32)).astype(jnp.bfloat16)

def mixer_output(gate_in, value_in, gate_out, conv_taps, prior_gate, prior_value):
    product = gate_in.astype(jnp.float32) * value_in.astype(jnp.float32)
    prior_mix = prior_gate.astype(jnp.float32) * prior_value.astype(jnp.float32)
    padded = jnp.concatenate([prior_mix, product], axis=0)
    taps = conv_taps.astype(jnp.float32)
    conv_sum = taps[0] * padded[:-2] + taps[1] * padded[1:-1] + taps[2] * padded[2:]
    return (gate_out.astype(jnp.float32) * conv_sum).astype(jnp.bfloat16)

def reference(gate_in, value_in, gate_out, conv_taps, proj_weight, residual, norm_gain, routes, route_weight, expert_gate, expert_up, expert_down):
    model_width = residual.shape[1]
    zero_rows = jnp.zeros((2, gate_in.shape[1]), jnp.bfloat16)
    mixed_out = mixer_output(gate_in, value_in, gate_out, conv_taps, zero_rows, zero_rows)
    slice_width = model_width // N_TP
    summed = jnp.zeros(residual.shape, jnp.float32)
    for group in range(N_TP):
        lower = group * slice_width
        summed = summed + rounded(jnp.dot(mixed_out[:, lower:lower + slice_width], proj_weight[lower:lower + slice_width], preferred_element_type=jnp.float32))
    hidden_rows = residual.astype(jnp.float32) + summed
    normed = normalize(hidden_rows, norm_gain)
    token_count = residual.shape[0]
    top_count = routes.shape[1]
    slots = slot_numbers(routes, TOKQ, EXPERTS)
    token_ids = jnp.arange(token_count, dtype=jnp.int32)
    source = token_ids // TOK_DEV
    quarter = token_ids % TOK_DEV // TOKQ
    flat_index = ((routes * N_TP + quarter[:, None]) * N_SP + source[:, None]) * CAPQ + slots
    per_expert = N_TP * N_SP * CAPQ
    slot_count = EXPERTS * per_expert
    slot_token = jnp.full((slot_count,), token_count, jnp.int32).at[flat_index.reshape(-1)].set(jnp.repeat(token_ids, top_count))
    slot_weight = jnp.zeros((slot_count,), jnp.float32).at[flat_index.reshape(-1)].set(route_weight.reshape(-1))
    padded_rows = jnp.concatenate([normed, jnp.zeros((1, model_width), jnp.bfloat16)], axis=0)
    hidden_width = expert_gate.shape[2] // N_TP

    def one_expert(total, expert):
        start_row = (expert * per_expert).astype(jnp.int32)
        chosen = lax.dynamic_slice_in_dim(slot_token, start_row, per_expert, 0)
        weights_now = lax.dynamic_slice_in_dim(slot_weight, start_row, per_expert, 0)
        row_block = padded_rows[chosen]
        gate_pre = jnp.dot(row_block, expert_gate[expert], preferred_element_type=jnp.float32)
        up_pre = jnp.dot(row_block, expert_up[expert], preferred_element_type=jnp.float32)
        hidden = (jax.nn.silu(gate_pre) * up_pre).astype(jnp.bfloat16)
        down_weight = expert_down[expert]
        partial_sum = jnp.zeros((per_expert, model_width), jnp.float32)
        for group in range(N_TP):
            lower = group * hidden_width
            partial_sum = partial_sum + rounded(jnp.dot(hidden[:, lower:lower + hidden_width], down_weight[lower:lower + hidden_width], preferred_element_type=jnp.float32))
        expert_rows = rounded(partial_sum)
        total = total.at[chosen].add(weights_now[:, None] * expert_rows)
        return (total, None)
    total, _ = lax.scan(one_expert, jnp.zeros((token_count + 1, model_width), jnp.float32), jnp.arange(EXPERTS, dtype=jnp.int32))
    return (hidden_rows + total[:token_count]).astype(jnp.bfloat16)
```

```python
import jax
import jax.numpy as jnp
from jax import lax
from jax.sharding import PartitionSpec as P


def swapped(values, axis, distance):
    size = lax.axis_size(axis)
    return lax.ppermute(values, axis, [(i, i ^ distance) for i in range(size)])


def passed_along(shard, axis, by):
    size = lax.axis_size(axis)
    pairs = [(i, i + by) for i in range(size) if 0 <= i + by < size]
    return lax.ppermute(shard, axis, pairs)


def product_of(left, right):
    return jnp.dot(left, right, preferred_element_type=jnp.float32)


def narrow(values):
    return values.astype(jnp.bfloat16)


def wide(values):
    return values.astype(jnp.float32)


def normalize(hidden_rows, norm_gain):
    inverse = lax.rsqrt(jnp.mean(hidden_rows * hidden_rows, axis=-1, keepdims=True) + 1e-05)
    return (hidden_rows * inverse * norm_gain).astype(jnp.bfloat16)


def body(
    gate_in,
    value_in,
    gate_out,
    conv_taps,
    proj_weight,
    residual,
    norm_gain,
    routes,
    route_weight,
    expert_gate,
    expert_up,
    expert_down,
):
    tok_dev = gate_in.shape[0]
    model_width = residual.shape[1]
    groups = lax.axis_size("sp")
    quarter = residual.shape[0]
    top_count = routes.shape[1]
    capacity = 2 * quarter * top_count // groups
    tp_index = lax.axis_index("tp")
    sp_index = lax.axis_index("sp")
    pairwise = groups <= 8

    halo = passed_along(
        jnp.concatenate([gate_in[tok_dev - 2 :], value_in[tok_dev - 2 :]], axis=0), "sp", 1
    )
    product = wide(gate_in) * wide(value_in)
    padded = jnp.concatenate([wide(halo[:2]) * wide(halo[2:]), product], axis=0)
    conv_sum = conv_taps[0] * padded[:-2] + conv_taps[1] * padded[1:-1] + conv_taps[2] * padded[2:]
    mixed_out = narrow(wide(gate_out) * conv_sum)

    def rows_for(distance):
        return lax.dynamic_slice_in_dim(mixed_out, (tp_index ^ distance) * quarter, quarter, 0)

    far = narrow(product_of(jnp.concatenate([rows_for(3), rows_for(2)], axis=0), proj_weight))
    far_other = swapped(far[:quarter], "tp", 1)
    far_sum = swapped(narrow(wide(far[quarter:]) + wide(far_other)), "tp", 2)
    near = narrow(product_of(jnp.concatenate([rows_for(1), rows_for(0)], axis=0), proj_weight))
    near_other = swapped(near[:quarter], "tp", 1)
    my_rows = wide(residual) + (wide(near[quarter:]) + wide(near_other) + wide(far_sum))
    normed = normalize(my_rows, norm_gain)

    own_routes = lax.dynamic_slice_in_dim(routes, tp_index * quarter, quarter, 0)
    own_weights = lax.dynamic_slice_in_dim(route_weight, tp_index * quarter, quarter, 0)
    experts = jnp.arange(groups, dtype=jnp.int32)
    if pairwise:
        experts = experts ^ sp_index
    named = own_routes.T[:, None, :] == experts[None, :, None]
    any_named = jnp.any(named, axis=0)
    token = jnp.arange(quarter, dtype=jnp.int32)
    earlier = (token[:, None] < token[None, :]).astype(jnp.bfloat16)
    slots = product_of(any_named.astype(jnp.bfloat16), earlier).astype(jnp.int32)
    slot = jnp.arange(capacity, dtype=jnp.int32)
    at_slot = slots[:, None, :] == slot[None, :, None]
    select = (any_named[:, None, :] & at_slot).astype(jnp.bfloat16)
    place = (named[:, :, None, :] & at_slot[None]).astype(jnp.bfloat16)

    gate_weight = expert_gate[0]
    up_weight = expert_up[0]
    down_weight = expert_down[0]

    def expert(rows):
        gate_pre = product_of(rows, gate_weight)
        up_pre = product_of(rows, up_weight)
        hidden = lax.optimization_barrier(narrow(jax.nn.silu(gate_pre) * up_pre))
        return narrow(product_of(hidden, down_weight))

    def gathered(own):
        across = swapped(own, "tp", 2)
        return (swapped(across, "tp", 1), across, swapped(own, "tp", 1), own)

    def scattered(rows, count):
        far_other = swapped(rows[:count], "tp", 1)
        far_part = narrow(wide(rows[count : 2 * count]) + wide(far_other))
        far_sum = swapped(far_part, "tp", 2)
        near_other = swapped(rows[2 * count : 3 * count], "tp", 1)
        return narrow(wide(rows[3 * count :]) + wide(near_other) + wide(far_sum))

    def send(pieces, first):
        if not pairwise:
            return lax.all_to_all(pieces, "sp", split_axis=0, concat_axis=0, tiled=True)
        moved = []
        for m in range(pieces.shape[0]):
            piece = pieces[m : m + 1]
            if first + m > 0:
                piece = swapped(piece, "sp", first + m)
            moved.append(piece)
        return jnp.concatenate(moved, axis=0)

    size = max(1, groups // 4) if pairwise else groups
    starts = list(range(0, groups, size))
    order = starts[:2] + starts[:1:-1]
    arrived = {}
    for first in order:
        chosen = select[first : first + size].reshape(size * capacity, quarter)
        outgoing = narrow(product_of(chosen, normed))
        arrived[first] = send(outgoing.reshape(size, capacity, model_width), first)
    results = {}
    for first in order:
        own = arrived[first].reshape(size * capacity, model_width)
        blocks = gathered(own)
        rows = expert(jnp.concatenate(blocks, axis=0))
        results[first] = scattered(rows, size * capacity)
    total = my_rows
    for first in order:
        returned = send(results[first].reshape(size, capacity, model_width), first)
        returned = returned.reshape(size * capacity, model_width)
        for k in range(top_count):
            chosen = place[k, first : first + size].reshape(size * capacity, quarter)
            picked = lax.dot_general(
                chosen, returned, (((0,), (0,)), ((), ())), preferred_element_type=jnp.float32
            )
            total = total + own_weights[:, k : k + 1] * picked
    return narrow(total)


def solution(mesh):
    placed = (
        P("sp", "tp"),
        P("sp", "tp"),
        P("sp", "tp"),
        P(None, "tp"),
        P("tp", None),
        P(("sp", "tp"), None),
        P(),
        P("sp", None),
        P("sp", None),
        P("sp", None, "tp"),
        P("sp", None, "tp"),
        P("sp", "tp", None),
    )

    return jax.shard_map(
        body, mesh=mesh, in_specs=placed, out_specs=P(("sp", "tp"), None), check_vma=False
    )
```
